32 devices in a mesh: kv: 16 (over z, y, x), tp: 2 (over core).
Axes of the slice: x: 2, y: 2, z: 4, core: 2. Of those that a mesh axis runs over, the one named last changes fastest.
Arguments:
- tokens: bfloat16 [64, 4096], P(None, 'kv'), may hold values from -160 to 160
- norm_gain: float32 [4096], P('kv'), may hold values from 0.1 to 1.9
- w_query: bfloat16 [4096, 2048], P('kv', 'tp'), may hold values from -0.09375 to 0.09375
- w_key: bfloat16 [4096, 2048], P('kv', 'tp'), may hold values from -0.5 to 0.5
- w_value: bfloat16 [4096, 2048], P('kv', 'tp'), may hold values from -0.09375 to 0.09375
- w_out: bfloat16 [2048, 4096], P('tp', 'kv'), may hold values from -0.125 to 0.125
- lambdas: float32 [16], P('tp'), may hold values from 0.3 to 0.8
- sub_gain: float32 [128], replicated, may hold values from 0.1 to 1.9
- key_cache: bfloat16 [4, 16, 8192, 128], P(None, 'tp', 'kv'), may hold values from -512 to 512
- value_cache: bfloat16 [4, 16, 8192, 128], P(None, 'tp', 'kv'), may hold values from -6 to 6
- prior: int32 [4], replicated, may hold values from 6144 to 8160
- accepted: int32 [4], replicated, may hold values from 1 to 16
- parent: int32 [4, 16], replicated, may hold values from -1 to 14, as said below
Outputs:
- mixed: bfloat16 [64, 4096], P('tp', 'kv')
- key_out: bfloat16 [4, 16, 8192, 128], P(None, 'tp', 'kv')
- value_out: bfloat16 [4, 16, 8192, 128], P(None, 'tp', 'kv')
The draws below stay inside these ranges and needn't reach their ends.
Inputs may be any that keep to these rules, and one draw needn't show every extreme that they name: parent[s, 0] is -1, and 0 <= parent[s, j] < j for j >= 1.
All inputs are finite; a program needn't handle non-finite values.
Results may differ from the reference program's by a relative error of at most 0.015.
The reference program's roundings to bfloat16 on the way count: a program that leaves them out, or rounds other values in their place, can miss the bound.
Values may be sent and summed in bfloat16 or wider, within the bound.
No kernel may reach another device: no remote copies, remote signals or barrier semaphores. Data moves between devices by JAX's collectives and lax.ppermute only.
A program may use at most 64 MiB of HBM per device.

```python
import jax
import jax.numpy as jnp
from jax import lax

D = 4096
HEADS = 16
HDIM = 64
VDIM = 128
SEQS = 4
PROPS = 16
CTX = 8192
TOKENS = 64
N_TP = 2


def draw_tokens(key, part):
    columns = jnp.arange(D, dtype=jnp.float32) / D
    row_power = jax.random.uniform(jax.random.fold_in(key, 3), (TOKENS, 1), jnp.float32, 0.0, 1.0)
    base = jnp.clip(jax.random.normal(jax.random.fold_in(key, 5), (TOKENS, D), jnp.float32), -4.0, 4.0)
    rising = 3.0 ** columns
    return (base * rising[None, :] * 10.0 ** row_power).astype(jnp.bfloat16)


def draw_key_cache(key, part):
    shape = (SEQS, HEADS, CTX, 2 * HDIM)
    base = 1.75 * jnp.clip(jax.random.normal(jax.random.fold_in(key, 7), shape, jnp.float32), -6.0, 6.0)
    return base.astype(jnp.bfloat16)


def draw_parent(key, part):
    offsets = jax.random.randint(jax.random.fold_in(key, 11), (SEQS, PROPS), 1, 5)
    positions = jnp.arange(PROPS, dtype=jnp.int32)[None, :]
    chosen = jnp.maximum(positions - offsets, 0)
    return jnp.where(positions == 0, -1, chosen).astype(jnp.int32)


def place_ends(values, key, smallest, largest):
    extent = values.shape
    index_at = [jax.random.randint(jax.random.fold_in(key, axis), (), 0, extent[axis]) for axis in range(len(extent))]
    values = values.at[tuple(index_at)].set(smallest)
    longest = extent.index(max(extent))
    index_at[longest] = (index_at[longest] + 1) % extent[longest]
    return values.at[tuple(index_at)].set(largest)


def shard_levels(own_key, dims, split, smallest, high):
    def one(axis_at, parts):
        draws = jax.random.uniform(jax.random.fold_in(jax.random.fold_in(own_key, 6), axis_at), (parts,), jnp.float32, smallest / len(split), high / len(split))
        return jnp.repeat(jnp.exp(draws), dims[axis_at] // parts).reshape((-1,) + (1,) * (len(dims) - axis_at - 1))

    level = one(*split[0])
    for cut in split[1:]:
        level = level * one(*cut)
    return level


def centred(rng, extent, scale, limit, cuts=(), held_as=jnp.bfloat16):
    gain = shard_levels(rng, extent, cuts, -0.22, 0.18) if cuts else 1.0
    result = jax.random.normal(rng, extent, jnp.float32) * scale * gain
    return jnp.minimum(jnp.maximum(result, -limit), limit).astype(held_as)


def setup_inputs(seed: int = 0) -> dict:
    splits = jax.random.split(jax.random.key(seed), 14)
    tokens = draw_tokens(jax.random.fold_in(splits[13], 71), 0)
    norm_gain = jnp.clip(1.0 + 0.18 * jax.random.normal(splits[1], (D,), jnp.float32), 0.1, 1.9)
    w_query = centred(splits[2], (D, HEADS * 2 * HDIM), D ** -0.5, 0.09375, ((0, 16), (1, 2)))
    w_key = centred(splits[3], (D, HEADS * 2 * HDIM), (D // 32) ** -0.5, 0.5, ((0, 16), (1, 2)))
    w_value = centred(splits[4], (D, HEADS * VDIM), D ** -0.5, 0.09375, ((0, 16), (1, 2)))
    w_out = centred(splits[5], (HEADS * VDIM, D), (HEADS * VDIM) ** -0.5, 0.125, ((0, 2), (1, 16)))
    lambdas = jnp.clip(0.3 + 0.5 * jax.random.uniform(splits[6], (HEADS,), jnp.float32) ** shard_levels(splits[6], (HEADS,), ((0, 2),), -0.2, 0.2), 0.3, 0.8)
    sub_gain = jnp.clip(1.0 + 0.18 * jax.random.normal(splits[7], (VDIM,), jnp.float32), 0.1, 1.9)
    key_cache = draw_key_cache(jax.random.fold_in(splits[13], 71), 0)
    value_cache = centred(splits[9], (SEQS, HEADS, CTX, VDIM), 1.0, 6.0, ((1, 2), (2, 16)))
    prior = place_ends(jax.random.randint(splits[10], (SEQS,), CTX * 3 // 4, CTX - 2 * PROPS + 1), jax.random.fold_in(splits[10], 1), CTX * 3 // 4, CTX - 2 * PROPS).astype(jnp.int32)
    accepted = place_ends(jax.random.randint(splits[11], (SEQS,), 1, PROPS + 1), jax.random.fold_in(splits[11], 1), 1, PROPS).astype(jnp.int32)
    parent = draw_parent(jax.random.fold_in(splits[13], 71), 0)
    return dict(tokens=tokens, norm_gain=norm_gain, w_query=w_query, w_key=w_key, w_value=w_value, w_out=w_out, lambdas=lambdas, sub_gain=sub_gain, key_cache=key_cache, value_cache=value_cache, prior=prior, accepted=accepted, parent=parent)


epsilon = 1e-06
masked_score = -1e+30
head_scale = 0.8

def ancestors(parent):
    prop_count = parent.shape[1]
    identity = jnp.eye(prop_count, dtype=jnp.float32)
    parent_hot = (parent[:, :, None] == jnp.arange(prop_count, dtype=jnp.int32)[None, None, :]).astype(jnp.float32)

    def extend(depth_step, ancestry):
        return identity[None] + jnp.einsum('sjm,smi->sji', parent_hot, ancestry, precision=lax.Precision.HIGHEST)
    return lax.fori_loop(0, prop_count, extend, jnp.broadcast_to(identity, parent_hot.shape))

def reference(tokens, norm_gain, w_query, w_key, w_value, w_out, lambdas, sub_gain, key_cache, value_cache, prior, accepted, parent):
    as_float = tokens.astype(jnp.float32)
    row_scale = lax.rsqrt(lax.optimization_barrier(jnp.mean(as_float * as_float, axis=1)) + epsilon)
    normed = (as_float * norm_gain[None, :]).astype(jnp.bfloat16)

    def project(weight_matrix):
        product = jnp.dot(normed, weight_matrix, preferred_element_type=jnp.float32)
        return (row_scale[:, None] * product).astype(jnp.bfloat16)
    queries = project(w_query).reshape(SEQS, PROPS, HEADS, 2, HDIM)
    new_key = project(w_key).reshape(SEQS, PROPS, HEADS, 2 * HDIM).transpose(0, 2, 1, 3)
    new_value = project(w_value).reshape(SEQS, PROPS, HEADS, VDIM).transpose(0, 2, 1, 3)
    valid_end = (prior + accepted).astype(jnp.int32)
    zero_index = jnp.int32(0)

    def write_rows(cache_seq, rows_seq, start):
        return lax.dynamic_update_slice(cache_seq, rows_seq, (zero_index, start.astype(jnp.int32), zero_index))
    key_out = jax.vmap(write_rows)(key_cache, new_key, valid_end)
    value_out = jax.vmap(write_rows)(value_cache, new_value, valid_end)
    ancestry = ancestors(parent)
    positions = jnp.arange(CTX, dtype=jnp.int32)
    prop_iota = jnp.arange(PROPS, dtype=jnp.int32)

    def attend_one(item):
        query_seq, keys_seq, values_seq, valid_seq, ancestry_seq = item
        offset_in = positions - valid_seq
        one_hot = (offset_in[:, None] == prop_iota[None, :]).astype(jnp.float32)
        in_tree = jnp.dot(ancestry_seq, one_hot.T, precision=lax.Precision.HIGHEST)
        allowed = (offset_in < 0)[None, :] | (in_tree > 0.5)
        visible = allowed[None, None]
        halves = keys_seq.astype(jnp.float32).reshape(HEADS, CTX, 2, HDIM)
        scores = jnp.einsum('jhmd,hpmd->mhjp', query_seq.astype(jnp.float32), halves) * HDIM ** (-0.5)
        maximum = lax.optimization_barrier(jnp.max(jnp.where(visible, scores, masked_score), axis=-1, keepdims=True))
        weight = jnp.where(visible, jnp.exp(scores - maximum), 0.0)
        totals = lax.optimization_barrier(jnp.sum(weight, axis=-1))
        rounded = lax.optimization_barrier(weight.astype(jnp.bfloat16)).astype(jnp.float32)
        summed = jnp.einsum('mhjp,hpc->mhjc', rounded, values_seq.astype(jnp.float32))
        head_out = summed[0] / totals[0][..., None] - lambdas[:, None, None] * summed[1] / totals[1][..., None]
        mean_square = lax.optimization_barrier(jnp.mean(head_out * head_out, axis=-1, keepdims=True))
        normed_head = head_out * lax.rsqrt(mean_square + epsilon) * sub_gain * head_scale
        return normed_head.transpose(1, 0, 2).astype(jnp.bfloat16)
    attended = lax.map(attend_one, (queries, key_out, value_out, valid_end, ancestry))
    group_size = HEADS // N_TP * VDIM
    attended = attended.reshape(TOKENS, N_TP, group_size)
    out_groups = w_out.reshape(N_TP, group_size, D)
    partial_value = jnp.einsum('tgc,gcd->gtd', attended.astype(jnp.float32), out_groups.astype(jnp.float32))
    partial_value = lax.optimization_barrier(partial_value.astype(jnp.bfloat16)).astype(jnp.float32)
    mixed = lax.optimization_barrier(jnp.sum(partial_value, axis=0)).astype(jnp.bfloat16)
    return (mixed, key_out, value_out)
```

```python
import functools

import jax
import jax.numpy as jnp
from jax import lax
from jax.experimental import pallas as pl
from jax.experimental.pallas import tpu as pltpu
from jax.sharding import PartitionSpec as P

epsilon = 1e-06
masked_score = -1e30
head_scale = 0.8
stat_rows = 8

VMEM = pl.BlockSpec(memory_space=pltpu.VMEM)
SMEM = pl.BlockSpec(memory_space=pltpu.SMEM)
HBM = pl.BlockSpec(memory_space=pltpu.HBM)
ANY = pl.BlockSpec(memory_space=pl.ANY)
small = pltpu.CompilerParams(vmem_limit_bytes=8 << 20)
large = pltpu.CompilerParams(vmem_limit_bytes=16 << 20)


def in_hbm(array):
    return pltpu.with_memory_space_constraint(array, pltpu.HBM)


def in_vmem(array):
    return pltpu.with_memory_space_constraint(array, pltpu.VMEM)


def pieces(value):
    high = value.astype(jnp.bfloat16).astype(jnp.float32)
    rest = value - high
    middle = rest.astype(jnp.bfloat16).astype(jnp.float32)
    return high, middle, rest - middle


def in_lanes(columns, lanes):
    rows = columns[0].shape[0]
    lane = lax.broadcasted_iota(jnp.int32, (rows, lanes), 1)
    result = jnp.zeros((rows, lanes), jnp.float32)
    for k, column in enumerate(columns):
        result = jnp.where(lane == k, column, result)
    return result


def turned_stats(maximum, totals, dim):
    rows = maximum.shape[0]
    stats = in_lanes(pieces(maximum) + pieces(totals), dim).astype(jnp.bfloat16)
    shape = (stat_rows, dim)
    pick = lax.broadcasted_iota(jnp.int32, shape, 0) == lax.broadcasted_iota(jnp.int32, shape, 1)
    pick = jnp.where(pick, 1.0, 0.0).astype(jnp.bfloat16)
    turned = lax.dot_general(
        pick, stats, (((1,), (1,)), ((), ())), preferred_element_type=jnp.float32
    )
    if rows < dim:
        padding = jnp.zeros((stat_rows, dim - rows), jnp.float32)
        turned = jnp.concatenate([turned, padding], axis=1)
    return turned


def side_by_side(queries, half):
    props, dim = queries[0].shape
    lane = lax.broadcasted_iota(jnp.int32, (props, dim), 1)
    zeros = jnp.zeros((props, dim), queries[0].dtype)
    blocks = []
    for m in range(2):
        for h, query in enumerate(queries):
            kept = jnp.where(lane < half if m == 0 else lane >= half, query, zeros)
            blocks.append(
                jnp.concatenate([kept if k == h else zeros for k in range(len(queries))], axis=1)
            )
    return jnp.concatenate(blocks, axis=0)


def score(queries, keys):
    half = queries[0].shape[1] // 2
    return lax.dot_general(
        side_by_side(queries, half),
        jnp.concatenate(keys, axis=1),
        (((1,), (1,)), ((), ())),
        preferred_element_type=jnp.float32,
    ) * half ** (-0.5)


def soften(masked):
    maximum = jnp.max(masked, axis=1, keepdims=True)
    weight = jnp.exp(masked - maximum)
    totals = jnp.sum(weight, axis=1, keepdims=True)
    return maximum, totals, weight.astype(jnp.bfloat16)


def weigh(weight, values, store):
    dim = values[0].shape[1]
    summed = jnp.dot(weight, jnp.concatenate(values, axis=1), preferred_element_type=jnp.float32)
    count = len(values)
    props = weight.shape[0] // (2 * count)
    for m in range(2):
        for k in range(count):
            first = (m * count + k) * props
            store(first, summed[first : first + props, k * dim : (k + 1) * dim])


def project_kernel(
    tokens_hbm, gain_hbm, w_query, w_key, w_value, out, tokens, gain, held, sems
):
    kv, each, whole = out.shape
    pairs = [(tokens_hbm, tokens), (gain_hbm, gain)]
    pairs += [(w, held.at[k]) for k, w in enumerate((w_query, w_key, w_value))]
    copies = [
        pltpu.make_async_copy(source, target, sems.at[k])
        for k, (source, target) in enumerate(pairs)
    ]
    for copy in copies:
        copy.start()
    copies[0].wait()
    copies[1].wait()
    as_float = tokens[...].astype(jnp.float32)
    squares = jnp.sum(as_float * as_float, axis=1, keepdims=True)
    normed = (as_float * gain[...]).astype(jnp.bfloat16)
    width = w_query.shape[1]
    last = whole - 3 * width
    stats = in_lanes(pieces(squares), last).astype(out.dtype)
    for i in range(kv):
        out[i, :, 3 * width :] = stats[i * each : (i + 1) * each]
    for k, copy in enumerate(copies[2:]):
        copy.wait()
        part = jnp.dot(normed, held[k], preferred_element_type=jnp.float32).astype(out.dtype)
        for i in range(kv):
            out[i, :, k * width : (k + 1) * width] = part[i * each : (i + 1) * each]


def reduce_kernel(features, parts, key_cache, value_cache, out):
    del key_cache, value_cache
    kv = parts.shape[0]
    width = out.shape[2]
    total = parts[0].astype(jnp.float32)
    for k in range(1, kv):
        total = total + parts[k].astype(jnp.float32)
    squares = jnp.sum(total[:, width : width + 3], axis=1, keepdims=True)
    scale = lax.rsqrt(squares / features + epsilon)
    done = (total[:, :width] * scale).astype(out.dtype)
    for k in range(kv):
        out[k] = done


def attend_kernel(
    layout,
    prior,
    accepted,
    qkv,
    keys,
    values,
    message,
    value_out,
    flat,
    scores,
    weights,
    held,
    out_sems,
    cache_sems,
):
    seqs, heads, length, dim = values.shape
    groups = layout.groups()
    leaving = []
    for s in range(seqs // 2):
        copy = pltpu.make_async_copy(values.at[s], value_out.at[s], cache_sems.at[s])
        copy.start()
        leaving.append(copy)
    kv, each = qkv.shape[:2]
    props = kv * each // seqs
    rows = 2 * layout.each * props
    for k in range(kv):
        flat[k * each : (k + 1) * each, :] = qkv[k, :, : heads * dim]
    for at, own in enumerate(groups):
        scores[at] = score(
            [flat[s * props : (s + 1) * props, h * dim : (h + 1) * dim] for s, h in own],
            [keys[s, h] for s, h in own],
        )
    stats = []
    ends = prior[...] + accepted[...] - lax.axis_index("kv") * length
    for at, own in enumerate(groups):
        end = [jnp.broadcast_to(ends[:, s : s + 1], (props, 1)) for s, _ in own]
        end = jnp.concatenate(end * 2, axis=0)
        visible = lax.broadcasted_iota(jnp.int32, (rows, length), 1) < end
        maximum, totals, weight = soften(jnp.where(visible, scores[at], masked_score))
        weights[at] = weight
        stats.append((maximum, totals))
    for at, (maximum, totals) in enumerate(stats):
        held[at, rows:, :] = turned_stats(maximum, totals, dim).astype(held.dtype)
    chunk = len(groups) // out_sems.shape[0]
    for at, own in enumerate(groups):

        def store(first, value, at=at):
            held[at, first : first + props, :] = value.astype(held.dtype)

        weigh(weights[at], [values[s, h] for s, h in own], store)
        if at % chunk == chunk - 1:
            part = pl.ds(at + 1 - chunk, chunk)
            copy = pltpu.make_async_copy(
                held.at[part], message.at[part], out_sems.at[at // chunk]
            )
            copy.start()
            leaving.append(copy)
    for copy in leaving:
        copy.wait()


def tree_kernel(
    layout,
    prior,
    accepted,
    parent,
    lambdas,
    sub_gain,
    qkv,
    key_cache,
    value_cache,
    value_out_in,
    own,
    second,
    key_out,
    value_out,
    flat,
    cached,
    windows,
    read_sems,
    sems,
):
    del value_out_in
    place = lax.axis_index("kv")
    seqs, heads, length, dim = key_cache.shape
    props = parent.shape[1]
    width = heads * dim
    span = 2 * props
    kv, each = qkv.shape[:2]
    reads, starts = [], []
    for s in range(seqs):
        end = prior[s] + accepted[s] - place * length
        start = jnp.clip((end // props) * props, 0, length - span)
        start = pl.multiple_of(start, props)
        starts.append((start, end))
        if s < seqs // 2:
            later = (value_cache.at[s, :, pl.ds(start, span), :], windows.at[s])
        else:
            later = (value_cache.at[s], cached.at[1, s])
        pairs = ((key_cache.at[s], cached.at[0, s]), later)
        for which, (source, target) in enumerate(pairs):
            copy = pltpu.make_async_copy(source, target, read_sems.at[which, s])
            copy.start()
            reads.append(copy)
    for k in range(kv):
        flat[k * each : (k + 1) * each, :] = qkv[k]
    rows = 2 * layout.each * props
    share = second.shape[0] - stat_rows
    split = layout.each * props // share
    mine = [layout.pair(place // split, k) for k in range(layout.each)]
    each = share // layout.each
    for k, (_, h) in enumerate(mine):
        second[k * each : (k + 1) * each, :] = jnp.full((each, dim), lambdas[h], jnp.float32)
    second[share:, :] = jnp.broadcast_to(sub_gain[...] * head_scale, (stat_rows, dim))
    row = lax.broadcasted_iota(jnp.int32, (props, props), 0)
    column = lax.broadcasted_iota(jnp.int32, (props, props), 1)
    reaches = []
    for s, _ in mine:
        above = jnp.full((props, props), -1, jnp.int32)
        for j in range(props):
            above = jnp.where(row == j, parent[s, j], above)
        reach = jnp.where((row == column) | (column == above), 1.0, 0.0)
        steps = 1
        while steps < props:
            now = reach.astype(jnp.bfloat16)
            reach = jnp.dot(now, now, preferred_element_type=jnp.float32)
            reach = jnp.where(reach > 0.5, 1.0, 0.0)
            steps *= 2
        reaches.append(reach)
    visible = jnp.concatenate(reaches * 2, axis=0) > 0.5

    def block(which, s, h):
        tokens = pl.ds(pl.multiple_of(s * props, props), props)
        first = pl.multiple_of(which * width + h * dim, dim)
        return flat[tokens, pl.ds(first, dim)]

    held = {}
    scores = score([block(0, s, h) for s, h in mine], [block(1, s, h) for s, h in mine])
    maximum, totals, weight = soften(jnp.where(visible, scores, masked_score))
    weigh(weight, [block(2, s, h) for s, h in mine], held.__setitem__)
    turned = turned_stats(maximum, totals, dim)
    if split == 1:
        for first, value in held.items():
            own[first : first + props, :] = value
        own[rows:, :] = turned
    else:
        part = place % split
        for k in range(split):

            @pl.when(part == k)
            def _(k=k):
                for m in range(2):
                    first = k * share
                    own[m * share : (m + 1) * share, :] = held[m * props][first : first + share]
                lanes = [turned[:, m * props + k * share :][:, :share] for m in range(2)]
                lanes.append(jnp.zeros((stat_rows, dim - 2 * share), jnp.float32))
                own[2 * share :, :] = jnp.concatenate(lanes, axis=1)

    writes = []
    for s in range(seqs):
        start, end = starts[s]
        offset = lax.broadcasted_iota(jnp.int32, (span, props), 0) + (start - end)
        hot = offset == lax.broadcasted_iota(jnp.int32, (span, props), 1)
        hot = jnp.where(hot, 1.0, 0.0).astype(jnp.bfloat16)
        offset = lax.broadcasted_iota(jnp.int32, (span, dim), 0) + (start - end)
        inside = (offset >= 0) & (offset < props)
        window = pl.ds(start, span)
        if s < seqs // 2:
            later = (windows.at[s], value_out.at[s, :, window, :])
        else:
            later = (cached.at[1, s], value_out.at[s])
        pairs = ((cached.at[0, s], key_out.at[s]), later)
        for which, (source, target) in enumerate(pairs):
            first = (1 + which) * width
            placed = jnp.dot(
                hot,
                flat[s * props : (s + 1) * props, first : first + width],
                preferred_element_type=jnp.float32,
            )
            reads[2 * s + which].wait()
            for h in range(heads):
                new = placed[:, h * dim : (h + 1) * dim]
                if which == 0 or s >= seqs // 2:
                    old = cached[which, s, h, window, :].astype(jnp.float32)
                    cached[which, s, h, window, :] = jnp.where(inside, new, old).astype(
                        cached.dtype
                    )
                else:
                    old = windows[s, h].astype(jnp.float32)
                    windows[s, h] = jnp.where(inside, new, old).astype(windows.dtype)
            copy = pltpu.make_async_copy(source, target, sems.at[which, s])
            copy.start()
            writes.append(copy)
    for copy in writes:
        copy.wait()


def merge_kernel(own, second, message, *rest):
    out = rest[-1]
    kv, rows, dim = message.shape
    count = own.shape[0] // 2 - stat_rows // 2
    both = 2 * count
    stats = message[:, both:, :].astype(jnp.float32)
    maximum = stats[:, 0:1, :] + stats[:, 1:2, :] + stats[:, 2:3, :]
    totals = stats[:, 3:4, :] + stats[:, 4:5, :] + stats[:, 5:6, :]
    stats = own[both:, :]
    own_maximum = stats[0:1, :] + stats[1:2, :] + stats[2:3, :]
    own_totals = stats[3:4, :] + stats[4:5, :] + stats[5:6, :]
    top = jnp.maximum(jnp.max(maximum, axis=0), own_maximum)
    factor = jnp.exp(maximum - top[None])
    own_factor = jnp.exp(own_maximum - top)
    whole = jnp.sum(totals * factor, axis=0) + own_totals * own_factor
    share = jnp.concatenate([(factor / whole[None]).reshape(kv, dim), own_factor / whole], axis=0)
    share = share.T
    summed = own[:both, :] * share[:both, kv : kv + 1]
    for k in range(kv):
        summed = summed + message[k, :both, :].astype(jnp.float32) * share[:both, k : k + 1]
    head_out = summed[:count] - second[:count, :] * summed[count:]
    mean_square = jnp.mean(head_out * head_out, axis=1, keepdims=True)
    attended = head_out * lax.rsqrt(mean_square + epsilon) * second[count : count + 1, :]
    attended = attended.astype(out.dtype)
    blocks, each = out.shape[:2]
    for k in range(blocks):
        first = k % (count // each) * each
        out[k] = attended[first : first + each]


def output_kernel(attended, w_out, out, held):
    seqs, heads, props, dim = attended.shape
    whole = jnp.concatenate(
        [
            jnp.concatenate([attended[s, h] for h in range(heads)], axis=1)
            for s in range(seqs)
        ],
        axis=0,
    )
    held[...] = jnp.dot(whole, w_out[...], preferred_element_type=jnp.float32).astype(out.dtype)
    parts, each = out.shape[:2]
    for k in range(parts):
        first = lax.rem(lax.axis_index("tp") + k, parts) * each
        out[k] = held[pl.ds(pl.multiple_of(first, each), each), :]


def mix_kernel(attended, *rest):
    weights, out = rest[:-1], rest[-1]
    tp = len(weights)
    heads = weights[0].shape[0] // attended.shape[2]
    total = None
    for k, weight in enumerate(weights):
        group = lax.rem(lax.axis_index("tp") + tp - k, tp)
        rows = []
        for s in range(attended.shape[0] // (tp * heads)):
            blocks = [attended[(s * heads + h) * tp + group] for h in range(heads)]
            rows.append(jnp.concatenate(blocks, axis=1))
        part = jnp.dot(
            jnp.concatenate(rows, axis=0), weight[...], preferred_element_type=jnp.float32
        )
        part = part.astype(out.dtype).astype(jnp.float32)
        total = part if total is None else total + part
    out[...] = total.astype(out.dtype)


class Layout:
    def __init__(self, seqs, heads, each, group_step, step):
        self.seqs, self.heads, self.each = seqs, heads, each
        self.group_step, self.step = group_step, step

    def pair(self, group, k):
        index = group * self.group_step + k * self.step
        return index // self.heads, index % self.heads

    def groups(self):
        count = self.seqs * self.heads // self.each
        return [[self.pair(g, k) for k in range(self.each)] for g in range(count)]


def row_of(vector):
    return vector.reshape(1, vector.shape[0])


def exchange(array, axes="kv"):
    return lax.all_to_all(array, axes, 0, 0)


def body(
    tokens,
    norm_gain,
    w_query,
    w_key,
    w_value,
    w_out,
    lambdas,
    sub_gain,
    key_cache,
    value_cache,
    prior,
    accepted,
    parent,
):
    kv, tp = lax.axis_size("kv"), lax.axis_size("tp")
    seqs, props = parent.shape
    heads = lambdas.shape[0]
    length, dim = key_cache.shape[2:]
    count, features = tokens.shape
    width = 3 * heads * dim
    bf16 = jnp.bfloat16

    parts = pl.pallas_call(
        project_kernel,
        out_shape=jax.ShapeDtypeStruct((kv, count // kv, width + dim), bf16),
        in_specs=[HBM] * 5,
        out_specs=VMEM,
        scratch_shapes=[
            pltpu.VMEM(tokens.shape, bf16),
            pltpu.VMEM((1, features), jnp.float32),
            pltpu.VMEM((3,) + w_query.shape, bf16),
            pltpu.SemaphoreType.DMA((5,)),
        ],
        compiler_params=small,
    )(*map(in_hbm, (tokens, row_of(norm_gain), w_query, w_key, w_value)))
    parts = exchange(parts)
    reduced = pl.pallas_call(
        functools.partial(reduce_kernel, features * kv),
        out_shape=jax.ShapeDtypeStruct((kv, count // kv, width), bf16),
        in_specs=[VMEM] + [HBM] * 2,
        out_specs=VMEM,
        compiler_params=small,
    )(parts, in_hbm(key_cache), in_hbm(value_cache))
    qkv = exchange(reduced)

    share = seqs * heads * props // kv
    heads_each = max(1, share // props)
    groups = seqs * heads // heads_each
    rows = 2 * heads_each * props
    by_tokens = heads_each == tp and share == tp * props and seqs % tp == 0
    if by_tokens:
        layout = Layout(seqs, heads, heads_each, 1, groups)
    else:
        layout = Layout(seqs, heads, heads_each, heads_each, 1)

    cache = pltpu.HBM(key_cache.shape, key_cache.dtype)
    message, value_out = pl.pallas_call(
        functools.partial(attend_kernel, layout),
        out_shape=(pltpu.HBM((groups, rows + stat_rows, dim), bf16), cache),
        in_specs=[VMEM] * 5,
        out_specs=(HBM, HBM),
        scratch_shapes=[
            pltpu.VMEM((count, width // 3), bf16),
            pltpu.VMEM((groups, rows, length), jnp.float32),
            pltpu.VMEM((groups, rows, length), bf16),
            pltpu.VMEM((groups, rows + stat_rows, dim), bf16),
            pltpu.SemaphoreType.DMA((4 if groups % 4 == 0 else 1,)),
            pltpu.SemaphoreType.DMA((seqs,)),
        ],
        compiler_params=small,
    )(row_of(prior), row_of(accepted), qkv, in_vmem(key_cache), in_vmem(value_cache))
    if share < props:
        split = props // share
        summed = message[:, :rows].reshape(groups, 2, split, share, dim)
        summed = summed.transpose(0, 2, 1, 3, 4).reshape(kv, 2 * share, dim)
        stats = message[:, rows:, :rows].reshape(groups, stat_rows, 2, split, share)
        stats = stats.transpose(0, 3, 1, 2, 4).reshape(kv, stat_rows, 2 * share)
        stats = jnp.pad(stats, ((0, 0), (0, 0), (0, dim - 2 * share)))
        message = jnp.concatenate([summed, stats], axis=1)
    message = exchange(message)
    own, second, key_out, value_out = pl.pallas_call(
        functools.partial(tree_kernel, layout),
        out_shape=(
            jax.ShapeDtypeStruct((2 * share + stat_rows, dim), jnp.float32),
            jax.ShapeDtypeStruct((share + stat_rows, dim), jnp.float32),
            cache,
            cache,
        ),
        in_specs=[SMEM] * 4 + [VMEM] * 2 + [HBM] * 3,
        out_specs=(VMEM, VMEM, HBM, HBM),
        scratch_shapes=[
            pltpu.VMEM((count, width), bf16),
            pltpu.VMEM((2,) + key_cache.shape, key_cache.dtype),
            pltpu.VMEM((seqs, heads, 2 * props, dim), bf16),
            pltpu.SemaphoreType.DMA((2, seqs)),
            pltpu.SemaphoreType.DMA((2, seqs)),
        ],
        input_output_aliases={8: 3},
        compiler_params=large,
    )(
        prior,
        accepted,
        parent,
        lambdas,
        row_of(sub_gain),
        qkv,
        *map(in_hbm, (key_cache, value_cache, value_out)),
    )
    blocks = (kv * tp, props, dim) if by_tokens else (kv, share, dim)
    columns = w_out.shape[1]
    rings = [[(i, (i + k) % tp) for i in range(tp)] for k in range(1, tp)]
    weights = [lax.ppermute(w_out, "tp", ring) for ring in rings] if by_tokens else []
    attended = pl.pallas_call(
        merge_kernel,
        out_shape=jax.ShapeDtypeStruct(blocks, bf16),
        in_specs=[VMEM] * 3 + [ANY] * len(weights),
        out_specs=VMEM,
        compiler_params=small,
    )(own, second, message, *weights)
    if by_tokens:
        mixed = pl.pallas_call(
            mix_kernel,
            out_shape=jax.ShapeDtypeStruct((count // tp, columns), bf16),
            in_specs=[VMEM] * (1 + tp),
            out_specs=VMEM,
            compiler_params=small,
        )(exchange(attended, ("kv", "tp")), w_out, *weights)
        return (mixed, key_out, value_out)
    partial_value = pl.pallas_call(
        output_kernel,
        out_shape=jax.ShapeDtypeStruct((tp, count // tp, columns), bf16),
        in_specs=[VMEM] * 2,
        out_specs=VMEM,
        scratch_shapes=[pltpu.VMEM((count, columns), bf16)],
        compiler_params=small,
    )(exchange(attended).reshape(seqs, heads, props, dim), w_out)
    mixed = partial_value[0].astype(jnp.float32)
    for k, ring in enumerate(rings):
        mixed = mixed + lax.ppermute(partial_value[k + 1], "tp", ring).astype(jnp.float32)
    return (mixed.astype(bf16), key_out, value_out)


def solution(mesh):
    return jax.shard_map(
        body,
        mesh=mesh,
        in_specs=(
            P(None, "kv"),
            P("kv"),
            P("kv", "tp"),
            P("kv", "tp"),
            P("kv", "tp"),
            P("tp", "kv"),
            P("tp"),
            P(),
            P(None, "tp", "kv", None),
            P(None, "tp", "kv", None),
            P(),
            P(),
            P(),
        ),
        out_specs=(P("tp", "kv"), P(None, "tp", "kv", None), P(None, "tp", "kv", None)),
        check_vma=False,
    )
```
